32 devices in a mesh: sp: 16 (over z, y, x), tp: 2 (over core).
Axes of the slice: x: 2, y: 2, z: 4, core: 2. Of those that a mesh axis runs over, the one named last changes fastest.
Arguments:
- tokens: bfloat16 [4096, 1024], P(('sp', 'tp')), may hold values from -16 to 16, as said below
- valid_len: int32 [1], replicated, may hold values from 3072 to 4096
- norm_gain: float32 [1024], replicated, may hold values from 0.5 to 1.5
- w_query: bfloat16 [1024, 4096], P(None, 'tp'), may hold values from -0.1875 to 0.1875
- w_key: bfloat16 [1024, 1024], P(None, 'tp'), may hold values from -0.1875 to 0.1875
- w_value: bfloat16 [1024, 1024], P(None, 'tp'), may hold values from -0.1875 to 0.1875
- q_gain: float32 [128], replicated, may hold values from 0.5 to 1.5
- k_gain: float32 [128], replicated, may hold values from 0.5 to 1.5
- w_out: bfloat16 [4096, 1024], P('tp'), may hold values from -0.375 to 0.375
Outputs:
- mixed: bfloat16 [4096, 1024], P(('sp', 'tp'))
The draws below stay inside these ranges and needn't reach their ends.
Inputs may be any that keep to these rules, and one draw needn't show every extreme that they name: tokens are random entries of unit-order spread (normal or uniform) plus a shift shared by every run of 256 consecutive rows, within -16 and 16. valid_len is at least three quarters of 4096 and at most 4096.
All inputs are finite; a program needn't handle non-finite values.
Results may differ from the reference program's by a relative error of at most 0.02.
Values may be sent and summed in bfloat16 or wider, within the bound.
A program may use at most 64 MiB of HBM per device.

```python
import jax
import jax.numpy as jnp
from jax import lax

D = 1024
HEAD_DIM = 128
KV_HEADS = 8
Q_PER_KV = 4
GRID_W = 64
TOK_DEV = 256
Q_HEADS = 32
TOKENS = 4096
N_SP = 16


def draw_tokens(key, part):
    noise_key = jax.random.fold_in(key, 11)
    shift_key = jax.random.fold_in(key, 12)
    groups = TOKENS // TOK_DEV
    noise_part = jax.random.normal(noise_key, (TOKENS, D), jnp.float32)
    shifts = 1.5 * jax.random.normal(shift_key, (groups, D), jnp.float32)
    shifted = noise_part + jnp.repeat(shifts, TOK_DEV, axis=0)
    return jnp.clip(shifted, -16.0, 16.0).astype(jnp.bfloat16)


def levels(rng, extent, cuts, low, top_value):
    def one(axis_at, parts):
        draws = jax.random.uniform(jax.random.fold_in(jax.random.fold_in(rng, 6), axis_at), (parts,), jnp.float32, low / len(cuts), top_value / len(cuts))
        return jnp.repeat(jnp.exp(draws), extent[axis_at] // parts).reshape((-1,) + (1,) * (len(extent) - axis_at - 1))

    level = one(*cuts[0])
    for cut in cuts[1:]:
        level = level * one(*cut)
    return level


def scatter_about(rng, dims, spread, limit, cuts=(), kind=jnp.bfloat16):
    level = levels(rng, dims, cuts, -0.22, 0.18) if cuts else 1.0
    drawn = jax.random.normal(rng, dims, jnp.float32) * spread * level
    return jnp.minimum(jnp.maximum(drawn, -limit), limit).astype(kind)


def setup_inputs(seed: int = 0) -> dict:
    seeds = jax.random.split(jax.random.key(seed), 10)
    tokens = draw_tokens(jax.random.fold_in(seeds[9], 71), 0)
    valid_len = jax.random.randint(seeds[1], (1,), TOKENS * 3 // 4, TOKENS + 1).astype(jnp.int32)
    norm_gain = jnp.clip(1.0 + 0.1 * jax.random.normal(seeds[2], (D,), jnp.float32), 0.5, 1.5)
    w_query = scatter_about(seeds[3], (D, Q_HEADS * HEAD_DIM), D ** -0.5, 0.1875, ((1, 2),))
    w_key = scatter_about(seeds[4], (D, KV_HEADS * HEAD_DIM), D ** -0.5, 0.1875, ((1, 2),))
    w_value = scatter_about(seeds[5], (D, KV_HEADS * HEAD_DIM), D ** -0.5, 0.1875, ((1, 2),))
    q_gain = jnp.clip(1.0 + 0.1 * jax.random.normal(seeds[6], (HEAD_DIM,), jnp.float32), 0.5, 1.5)
    k_gain = jnp.clip(1.0 + 0.1 * jax.random.normal(seeds[7], (HEAD_DIM,), jnp.float32), 0.5, 1.5)
    w_out = scatter_about(seeds[8], (Q_HEADS * HEAD_DIM, D), (Q_HEADS * HEAD_DIM // 16) ** -0.5, 0.375, ((0, 2),))
    return dict(tokens=tokens, valid_len=valid_len, norm_gain=norm_gain, w_query=w_query, w_key=w_key, w_value=w_value, q_gain=q_gain, k_gain=k_gain, w_out=w_out)


norm_eps = 1e-06
rope_base = 10000.0

def normalize(values, gain):
    scaled = values.astype(jnp.float32)
    return scaled * lax.rsqrt(lax.optimization_barrier(jnp.mean(scaled * scaled, axis=-1, keepdims=True)) + norm_eps) * gain

def rope_tables(positions, head_width):
    quarter = head_width // 4
    half_width = head_width // 2
    frequency = rope_base ** (-(jnp.arange(quarter, dtype=jnp.float32) * 2.0) / half_width)
    grid_row = (positions // GRID_W).astype(jnp.float32)
    grid_col = (positions % GRID_W).astype(jnp.float32)
    row_angle = grid_row[:, None] * frequency[None, :]
    col_angle = grid_col[:, None] * frequency[None, :]
    angles = jnp.concatenate([row_angle, row_angle, col_angle, col_angle], axis=-1)
    return (jnp.cos(angles), jnp.sin(angles))

def turn_half(values):
    width = values.shape[-1] // 2
    return jnp.concatenate([-values[..., width:], values[..., :width]], axis=-1)

def prepare(projected, gain, positions, factor):
    head_width = gain.shape[0]
    shaped = projected.astype(jnp.float32).reshape(projected.shape[0], -1, head_width)
    unit = normalize(shaped, gain)
    half_width = head_width // 2
    turned = jnp.concatenate([turn_half(unit[..., :half_width]), turn_half(unit[..., half_width:])], axis=-1)
    cosine, sine_table = rope_tables(positions, head_width)
    result = unit * cosine[:, None, :] + turned * sine_table[:, None, :]
    return (result * factor).astype(jnp.bfloat16)

def reference(tokens, valid_len, norm_gain, w_query, w_key, w_value, q_gain, k_gain, w_out):
    normed = normalize(tokens, norm_gain).astype(jnp.bfloat16)
    queries = jnp.dot(normed, w_query, preferred_element_type=jnp.float32).astype(jnp.bfloat16)
    keys_all = jnp.dot(normed, w_key, preferred_element_type=jnp.float32).astype(jnp.bfloat16)
    values = jnp.dot(normed, w_value, preferred_element_type=jnp.float32).astype(jnp.bfloat16)
    positions = jnp.arange(TOKENS, dtype=jnp.int32)
    turned_query = lax.optimization_barrier(prepare(queries, q_gain, positions, HEAD_DIM ** (-0.5)))
    turned_key = lax.optimization_barrier(prepare(keys_all, k_gain, positions, 1.0))
    key_wide = turned_key.astype(jnp.float32)
    value_wide = values.reshape(TOKENS, KV_HEADS, HEAD_DIM).astype(jnp.float32)
    key_valid = positions < valid_len[0]
    grouped = turned_query.reshape(N_SP, TOK_DEV, KV_HEADS, Q_PER_KV, HEAD_DIM)

    def attend(query_block):
        scores = jnp.einsum('qgrd,kgd->grqk', query_block.astype(jnp.float32), key_wide)
        scores = jnp.where(key_valid[None, None, None, :], scores, -jnp.inf)
        top = lax.optimization_barrier(jnp.max(scores, axis=-1, keepdims=True))
        weights = jnp.exp(scores - top)
        totals = lax.optimization_barrier(jnp.sum(weights, axis=-1))
        rounded = lax.optimization_barrier(weights.astype(jnp.bfloat16))
        summed = jnp.einsum('grqk,kgd->grqd', rounded.astype(jnp.float32), value_wide)
        result = summed / totals[..., None]
        return result.transpose(2, 0, 1, 3).reshape(TOK_DEV, Q_HEADS * HEAD_DIM).astype(jnp.bfloat16)
    attended = lax.map(attend, grouped).reshape(TOKENS, Q_HEADS * HEAD_DIM)
    return jnp.dot(attended, w_out, preferred_element_type=jnp.float32).astype(jnp.bfloat16)
```

```python
import functools
import math

import jax
import jax.numpy as jnp
from jax import lax
from jax.experimental import pallas as pl
from jax.experimental.pallas import tpu as pltpu
from jax.sharding import PartitionSpec as P

HEAD_DIM = 128
Q_PER_KV = 4
GRID_W = 64
CHUNK_BLOCKS = 2
FUSED = True

norm_eps = 1e-06
rope_base = 10000.0


def angle_tables(index, head_width, halves):
    quarter = head_width // 4
    frequency = rope_base ** (-(jnp.arange(quarter, dtype=jnp.float32) * 2.0) / (head_width // 2))
    angle = index.astype(jnp.float32)[:, None] * frequency[None, :]
    cosine, sine, zero = jnp.cos(angle), jnp.sin(angle), jnp.zeros_like(angle)
    blank = [zero, zero]

    def lay(pair):
        return jnp.concatenate(pair + blank if halves == 0 else blank + pair, axis=-1)

    return jnp.stack([lay([cosine, cosine]), lay([zero, sine]), lay([-sine, zero])])


def with_gain(tables, gain, factor):
    quarter = gain.shape[0] // 4
    gains = jnp.stack([gain, jnp.roll(gain, quarter), jnp.roll(gain, -quarter)])
    return tables * (gains * factor)[:, None, :]


def unit_rows(rows, gain):
    wide = rows.astype(jnp.float32)
    scale = lax.rsqrt(jnp.mean(wide * wide, axis=-1, keepdims=True) + norm_eps)
    return (wide * scale * gain).astype(jnp.bfloat16)


def rotate(part, tables):
    width = part.shape[-1]
    scale = lax.rsqrt(jnp.mean(part * part, axis=-1, keepdims=True) + norm_eps)
    ahead = pltpu.roll(part, width // 4, 1)
    behind = pltpu.roll(part, width - width // 4, 1)
    return (part * tables[0] + ahead * tables[1] + behind * tables[2]) * scale


def project_queries(own, gain_ref, w_query_ref, q_tab_ref, q_scr, block_rows):
    groups = q_scr.shape[0]
    normed = unit_rows(own, gain_ref[...])
    tables = [q_tab_ref[i] for i in range(3)]
    span = Q_PER_KV * HEAD_DIM
    for g in range(groups):
        projected = jnp.dot(
            normed, w_query_ref[:, g * span:(g + 1) * span], preferred_element_type=jnp.float32
        )
        for r in range(Q_PER_KV):
            head = rotate(projected[:, r * HEAD_DIM:(r + 1) * HEAD_DIM], tables)
            q_scr[g, r * block_rows:(r + 1) * block_rows, :] = head.astype(jnp.bfloat16)


def fold_chunk(start, chunk, tok_ref, valid_ref, gain_ref, w_key_ref, w_value_ref, row_tab_ref,
               col_tab_ref, q_scr, key_scr, val_scr, acc_scr, block_rows):
    groups = q_scr.shape[0]
    normed = unit_rows(tok_ref[pl.ds(start, chunk), :], gain_ref[...])
    keys = jnp.dot(normed, w_key_ref[...], preferred_element_type=jnp.float32)
    grid_rows = chunk // GRID_W
    first = pl.multiple_of(start // GRID_W, grid_rows)
    tables = []
    for i in range(3):
        rows = row_tab_ref[i, pl.ds(first, grid_rows), :]
        cols = col_tab_ref[i]
        tables.append(jnp.concatenate([rows[j:j + 1] + cols for j in range(grid_rows)], axis=0))
    for g in range(groups):
        turned = rotate(keys[:, g * HEAD_DIM:(g + 1) * HEAD_DIM], tables)
        key_scr[g] = turned.T.astype(jnp.bfloat16)
    values = jnp.dot(normed, w_value_ref[...], preferred_element_type=jnp.float32)
    at = start + lax.broadcasted_iota(jnp.int32, (chunk, HEAD_DIM), 0)
    kept = at < valid_ref[0]
    ones = jnp.where(kept, 1.0, 0.0).astype(jnp.bfloat16)
    for g in range(groups):
        part = values[:, g * HEAD_DIM:(g + 1) * HEAD_DIM]
        val_scr[g, :, :HEAD_DIM] = jnp.where(kept, part, 0.0).astype(jnp.bfloat16)
        val_scr[g, :, HEAD_DIM:] = ones

    def one_group(g, carry):
        for r in range(Q_PER_KV):
            span = slice(r * block_rows, (r + 1) * block_rows)
            scores = jnp.dot(q_scr[g, span, :], key_scr[g], preferred_element_type=jnp.float32)
            weights = jnp.exp2(scores).astype(jnp.bfloat16)
            acc_scr[g, span, :] += jnp.dot(
                weights, val_scr[g], preferred_element_type=jnp.float32
            )
        return carry

    lax.fori_loop(0, groups, one_group, 0)


def mix_heads(acc_scr, att_scr, block_rows):
    groups = acc_scr.shape[0]
    for g in range(groups):
        for r in range(Q_PER_KV):
            part = acc_scr[g, r * block_rows:(r + 1) * block_rows, :]
            head = g * Q_PER_KV + r
            att_scr[:, head * HEAD_DIM:(head + 1) * HEAD_DIM] = (
                part[:, :HEAD_DIM] / part[:, HEAD_DIM:]
            ).astype(jnp.bfloat16)


def local_kernel(block_rows, valid_ref, own_ref, tok_ref, gain_ref, w_query_ref, w_key_ref,
                 w_value_ref, w_out_ref, q_tab_ref, row_tab_ref, col_tab_ref, out_ref,
                 q_scr, key_scr, val_scr, acc_scr, att_scr):
    chunk = key_scr.shape[2]
    project_queries(own_ref[...], gain_ref, w_query_ref, q_tab_ref, q_scr, block_rows)
    acc_scr[...] = jnp.zeros_like(acc_scr)

    def step(i, carry):
        start = pl.multiple_of(i * chunk, chunk)
        fold_chunk(start, chunk, tok_ref, valid_ref, gain_ref, w_key_ref, w_value_ref,
                   row_tab_ref, col_tab_ref, q_scr, key_scr, val_scr, acc_scr, block_rows)
        return carry

    lax.fori_loop(0, tok_ref.shape[0] // chunk, step, 0)
    mix_heads(acc_scr, att_scr, block_rows)
    out_ref[...] = jnp.dot(
        att_scr[...], w_out_ref[...], preferred_element_type=jnp.float32
    ).astype(jnp.bfloat16)


def line_place(k, z, length):
    upper = (2 * z) // length
    near = z + upper * (length - 1 - 2 * z)
    far = (k + 1) // 2
    side = 2 * (k % 2) - 1
    beyond = jnp.minimum(k // (2 * near + 1), 1)
    mirrored = beyond * k + (1 - beyond) * (near + side * far)
    return mirrored + upper * (length - 1 - 2 * mirrored)


def fused_kernel(block_rows, total_sp, valid_ref, own_ref, gain_ref, w_query_ref, w_key_ref,
                 w_value_ref, w_out_ref, q_tab_ref, row_tab_ref, col_tab_ref, out_ref,
                 tok_ref, q_scr, key_scr, val_scr, acc_scr, att_scr, give_scr, take_scr,
                 col_recv, x_recv, y_recv, xd_recv, yd_recv, mate_recv,
                 up_send, down_send, x_send, y_send, xd_send, yd_send, mate_send, last_sem):
    chunk = key_scr.shape[2]
    half = block_rows // 2
    quart = half // 2
    length = total_sp // 4
    me = lax.axis_index("sp")
    core = lax.axis_index("tp")
    z, y, x = me // 4, (me // 2) % 2, me % 2
    x_mate = me + 1 - 2 * x
    y_mate = me + 2 - 4 * y
    d_mate = x_mate + 2 - 4 * y
    x_at, y_at, d_at = x_mate - 4 * z, y_mate - 4 * z, d_mate - 4 * z
    me_at = me - 4 * z

    def row_of(chip, which):
        return pl.multiple_of((chip * 2 + which) * half, half)

    def copy(row, count, device, send, recv, source=None):
        row = pl.multiple_of(row, count)
        here = tok_ref.at[pl.ds(row, count), :]
        return pltpu.make_async_remote_copy(
            src_ref=here if source is None else source,
            dst_ref=here,
            send_sem=send,
            recv_sem=recv,
            device_id=device,
            device_id_type=pl.DeviceIdType.MESH,
        )

    to_mate = {"sp": me, "tp": 1 - core}
    to_x = {"sp": x_mate, "tp": core}
    to_y = {"sp": y_mate, "tp": core}
    to_up = {"sp": me + 4, "tp": core}
    to_down = {"sp": me - 4, "tp": core}

    barrier = pltpu.get_barrier_semaphore()

    def greet(device):
        pl.semaphore_signal(barrier, inc=1, device_id=device, device_id_type=pl.DeviceIdType.MESH)

    greet(to_mate)
    greet(to_x)
    greet(to_y)

    @pl.when(z < length - 1)
    def _():
        greet(to_up)

    @pl.when(z > 0)
    def _():
        greet(to_down)

    has_up = jnp.minimum(length - 1 - z, 1)
    has_down = jnp.minimum(z, 1)
    pl.semaphore_wait(barrier, 3 + has_up + has_down)

    def mate_copy(chip, source=None):
        return copy(row_of(chip, core), half, to_mate, mate_send.at[chip], mate_recv.at[chip],
                    source)

    def mate_wait(chip):
        copy(row_of(chip, 1 - core), half, to_mate, mate_send.at[chip],
             mate_recv.at[chip]).wait_recv()

    def up_copy(layer, source=None):
        return copy(row_of(4 * layer + me_at, core), half, to_up, up_send.at[layer],
                    col_recv.at[layer], source)

    def down_copy(layer, source=None):
        return copy(row_of(4 * layer + me_at, core), half, to_down, down_send.at[layer],
                    col_recv.at[layer], source)

    def x_copy(layer, source=None):
        return copy(row_of(4 * layer + me_at, core), half, to_x, x_send.at[layer],
                    x_recv.at[layer], source)

    def y_copy(layer, source=None):
        return copy(row_of(4 * layer + me_at, core), half, to_y, y_send.at[layer],
                    y_recv.at[layer], source)

    def yd_copy(layer, at):
        return copy(row_of(4 * layer + at, core), quart, to_y, yd_send.at[layer],
                    yd_recv.at[layer])

    def xd_copy(layer, at):
        return copy(row_of(4 * layer + at, core) + quart, quart, to_x, xd_send.at[layer],
                    xd_recv.at[layer])

    def spread(layer, source=None):
        @pl.when(jnp.logical_and(layer <= z, z < length - 1))
        def _():
            up_copy(layer, source).start()

        @pl.when(jnp.logical_and(layer >= z, z > 0))
        def _():
            down_copy(layer, source).start()

        x_copy(layer, source).start()
        y_copy(layer, source).start()
        mate_copy(4 * layer + me_at, source).start()

    spread(z, own_ref)
    tok_ref[pl.ds(row_of(me, core), half), :] = own_ref[...]
    acc_scr[...] = jnp.zeros_like(acc_scr)
    mate_wait(me)
    project_queries(tok_ref[pl.ds(row_of(me, 0), block_rows), :], gain_ref, w_query_ref,
                    q_tab_ref, q_scr, block_rows)

    def fold(start):
        fold_chunk(start, chunk, tok_ref, valid_ref, gain_ref, w_key_ref, w_value_ref,
                   row_tab_ref, col_tab_ref, q_scr, key_scr, val_scr, acc_scr, block_rows)

    def step(k, carry):
        layer = line_place(k, z, length)
        copy(row_of(4 * layer + x_at, core), half, to_x, x_send.at[layer],
             x_recv.at[layer]).wait_recv()
        yd_copy(layer, x_at).start()
        mate_copy(4 * layer + x_at).start()
        copy(row_of(4 * layer + y_at, core), half, to_y, y_send.at[layer],
             y_recv.at[layer]).wait_recv()
        xd_copy(layer, y_at).start()
        mate_copy(4 * layer + y_at).start()

        @pl.when(k < length - 1)
        def _():
            later = line_place(k + 1, z, length)
            copy(row_of(4 * later + me_at, core), half, to_x, x_send.at[later],
                 col_recv.at[later]).wait_recv()
            spread(later)

        @pl.when(k > 0)
        def _():
            mate_wait(4 * layer + me_at)

        mate_wait(4 * layer + x_at)
        fold(pl.multiple_of((4 * layer + 2 * y) * block_rows, chunk))
        yd_copy(layer, d_at).wait_recv()
        xd_copy(layer, d_at).wait_recv()
        mate_copy(4 * layer + d_at).start()
        mate_wait(4 * layer + y_at)
        mate_wait(4 * layer + d_at)
        fold(pl.multiple_of((4 * layer + 2 - 2 * y) * block_rows, chunk))
        return carry

    lax.fori_loop(0, length, step, 0)
    mix_heads(acc_scr, att_scr, block_rows)

    theirs = pl.multiple_of((1 - core) * half, half)
    mine = pl.multiple_of(core * half, half)
    give_scr[...] = jnp.dot(
        att_scr[pl.ds(theirs, half), :], w_out_ref[...], preferred_element_type=jnp.float32
    ).astype(jnp.bfloat16)
    last = pltpu.make_async_remote_copy(
        src_ref=give_scr,
        dst_ref=take_scr,
        send_sem=last_sem.at[0],
        recv_sem=last_sem.at[1],
        device_id=to_mate,
        device_id_type=pl.DeviceIdType.MESH,
    )
    last.start()
    kept = jnp.dot(
        att_scr[pl.ds(mine, half), :], w_out_ref[...], preferred_element_type=jnp.float32
    )

    def settle(layer, carry):
        @pl.when(jnp.logical_and(layer <= z, z < length - 1))
        def _():
            up_copy(layer).wait_send()

        @pl.when(jnp.logical_and(layer >= z, z > 0))
        def _():
            down_copy(layer).wait_send()

        x_copy(layer).wait_send()
        y_copy(layer).wait_send()
        xd_copy(layer, y_at).wait_send()
        yd_copy(layer, x_at).wait_send()
        for at in range(4):
            mate_copy(4 * layer + at).wait_send()
        return carry

    lax.fori_loop(0, length, settle, 0)
    last.wait()
    out_ref[...] = (kept + take_scr[...].astype(jnp.float32)).astype(jnp.bfloat16)


def on_device(tokens, valid_len, norm_gain, w_query, w_key, w_value, q_gain, k_gain, w_out):
    head_width = q_gain.shape[0]
    local_rows, model_width = tokens.shape
    total_sp, total_tp = lax.axis_size("sp"), lax.axis_size("tp")
    block_rows = local_rows * total_tp
    all_rows = block_rows * total_sp
    groups = w_key.shape[1] // head_width
    chunk = CHUNK_BLOCKS * block_rows
    positions = lax.axis_index("sp") * block_rows + jnp.arange(block_rows, dtype=jnp.int32)
    q_factor = HEAD_DIM ** (-0.5) * math.log2(math.e)
    q_tables = with_gain(
        angle_tables(positions // GRID_W, head_width, 0)
        + angle_tables(positions % GRID_W, head_width, 1),
        q_gain, q_factor)
    row_tables = with_gain(
        angle_tables(jnp.arange(all_rows // GRID_W), head_width, 0), k_gain, 1.0)
    col_tables = with_gain(angle_tables(jnp.arange(GRID_W), head_width, 1), k_gain, 1.0)
    gain = norm_gain[None, :]
    vmem = pl.BlockSpec(memory_space=pltpu.VMEM)
    smem = pl.BlockSpec(memory_space=pltpu.SMEM)
    work = [
        pltpu.VMEM((groups, Q_PER_KV * block_rows, head_width), jnp.bfloat16),
        pltpu.VMEM((groups, head_width, chunk), jnp.bfloat16),
        pltpu.VMEM((groups, chunk, 2 * head_width), jnp.bfloat16),
        pltpu.VMEM((groups, Q_PER_KV * block_rows, 2 * head_width), jnp.float32),
        pltpu.VMEM((block_rows, groups * Q_PER_KV * head_width), jnp.bfloat16),
    ]
    if FUSED and total_tp == 2 and total_sp % 4 == 0:
        length = total_sp // 4
        dma = pltpu.SemaphoreType.DMA
        return pl.pallas_call(
            functools.partial(fused_kernel, block_rows, total_sp),
            out_shape=jax.ShapeDtypeStruct((local_rows, model_width), jnp.bfloat16),
            in_specs=[smem] + [vmem] * 9,
            out_specs=vmem,
            scratch_shapes=[pltpu.VMEM((all_rows, model_width), jnp.bfloat16)] + work + [
                pltpu.VMEM((local_rows, model_width), jnp.bfloat16),
                pltpu.VMEM((local_rows, model_width), jnp.bfloat16),
            ] + [dma((length,))] * 5 + [dma((total_sp,))] + [dma((length,))] * 6
            + [dma((total_sp,)), dma((2,))],
            compiler_params=pltpu.CompilerParams(
                collective_id=0, has_side_effects=True, vmem_limit_bytes=60 * 1024 * 1024),
        )(valid_len, tokens, gain, w_query, w_key, w_value, w_out, q_tables, row_tables,
          col_tables)
    gathered = lax.all_gather(tokens, ("sp", "tp"), axis=0, tiled=True)
    own = lax.dynamic_slice_in_dim(gathered, lax.axis_index("sp") * block_rows, block_rows, 0)
    partial = pl.pallas_call(
        functools.partial(local_kernel, block_rows),
        out_shape=jax.ShapeDtypeStruct((block_rows, model_width), jnp.bfloat16),
        in_specs=[smem] + [vmem] * 10,
        out_specs=vmem,
        scratch_shapes=work,
        compiler_params=pltpu.CompilerParams(vmem_limit_bytes=60 * 1024 * 1024),
    )(valid_len, own, gathered, gain, w_query, w_key, w_value, w_out, q_tables, row_tables,
      col_tables)
    return lax.psum_scatter(partial, "tp", scatter_dimension=0, tiled=True)


def solution(mesh):
    return jax.shard_map(
        on_device,
        mesh=mesh,
        in_specs=(
            P(("sp", "tp"), None),
            P(),
            P(),
            P(None, "tp"),
            P(None, "tp"),
            P(None, "tp"),
            P(),
            P(),
            P("tp", None),
        ),
        out_specs=P(("sp", "tp"), None),
        check_vma=False,
    )
```
